32 devices in a mesh: sp: 8 (over z, y), tp: 4 (over x, core).
Axes of the slice: x: 2, y: 2, z: 4, core: 2. Of those that a mesh axis runs over, the one named last changes fastest.
Arguments:
- activity: bfloat16 [2048, 4096], P('sp', 'tp'), may hold values from -8 to 8
- query_weight: bfloat16 [4096, 3072], P('sp', 'tp'), may hold values from -0.09375 to 0.09375
- key_weight: bfloat16 [4096, 3072], P('sp', 'tp'), may hold values from -0.09375 to 0.09375
- value_weight: bfloat16 [4096, 3072], P('sp', 'tp'), may hold values from -0.09375 to 0.09375
- merge_weight: bfloat16 [1024, 4096], P('tp', 'sp'), may hold values from -1.5 to 1.5
Outputs:
- attended: bfloat16 [2048, 4096], P(('sp', 'tp'))
The draws below stay inside these ranges and needn't reach their ends.
All inputs are finite; a program needn't handle non-finite values.
Results may differ from the reference program's by a relative error of at most 0.013.
Values may be sent and summed in bfloat16 or wider, within the bound.
No kernel may reach another device: no remote copies, remote signals or barrier semaphores. Data moves between devices by JAX's collectives and lax.ppermute only.
A program may use at most 128 MiB of HBM per device.

```python
import jax
import jax.numpy as jnp
from jax import lax

D = 4096
HPG = 16
HEAD = 64
HEAD_GROUPS = 3
SPAN = 128
DILATION_MIDDLE = 4
DILATION_WIDEST = 8
TOK_DEV = 256
TOKENS = 2048


def draw_activity(key, part):
    key_base, key_sign = jax.random.split(key, 2)
    drawn = jnp.clip(jax.random.normal(key_base, (TOKENS, D), jnp.float32), -6.0, 6.0)
    return drawn.astype(jnp.bfloat16)


def paired_weights(key):
    key_query = jax.random.fold_in(key, 11)
    key_other = jax.random.fold_in(key, 23)
    col_total = HEAD_GROUPS * HPG * HEAD
    weight_scale = D ** (-0.5)
    query_draw = jnp.clip(jax.random.normal(key_query, (D, col_total), jnp.float32), -6.0, 6.0) * weight_scale
    key_draw = jnp.clip(jax.random.normal(key_other, (D, col_total), jnp.float32), -6.0, 6.0) * weight_scale
    return (query_draw, key_draw)


def draw_query_weight(key, part):
    return paired_weights(key)[0].astype(jnp.bfloat16)


def draw_key_weight(key, part):
    return paired_weights(key)[1].astype(jnp.bfloat16)


def shard_levels(stream_key, extent, cuts, smallest, largest):
    def one(position, parts):
        heights = jax.random.uniform(jax.random.fold_in(jax.random.fold_in(stream_key, 6), position), (parts,), jnp.float32, smallest / len(cuts), largest / len(cuts))
        return jnp.repeat(jnp.exp(heights), extent[position] // parts).reshape((-1,) + (1,) * (len(extent) - position - 1))

    gain = one(*cuts[0])
    for cut in cuts[1:]:
        gain = gain * one(*cut)
    return gain


def noise(key, shape, width, reach, pieces=(), kind=jnp.bfloat16):
    values = jax.random.normal(key, shape, jnp.float32) * width
    if len(pieces) > 0:
        values = shard_levels(key, shape, pieces, -0.22, 0.18) * values
    return jnp.clip(values, min=-reach, max=reach).astype(kind)


def setup_inputs(seed: int = 0) -> dict:
    splits = jax.random.split(jax.random.key(seed), 6)
    activity = draw_activity(jax.random.fold_in(splits[5], 71), 0)
    query_weight = draw_query_weight(jax.random.fold_in(splits[5], 71), 0)
    key_weight = draw_key_weight(jax.random.fold_in(splits[5], 71), 0)
    value_weight = noise(splits[3], (D, HEAD_GROUPS * HPG * HEAD), D ** -0.5, 0.09375, ((0, 8), (1, 4)))
    merge_weight = noise(splits[4], (HPG * HEAD, D), (HEAD // 4) ** -0.5, 1.5, ((0, 4), (1, 8)))
    return dict(activity=activity, query_weight=query_weight, key_weight=key_weight, value_weight=value_weight, merge_weight=merge_weight)


rope_base = 500000.0


def rotate(channels, angle_pos):
    half_width = channels.shape[-1] // 2
    frequency = rope_base ** (-jnp.arange(0, half_width, dtype=jnp.float32) * 2.0 / channels.shape[-1])
    angles = angle_pos[:, None] * frequency[None, :]
    cosine = jnp.cos(angles)[:, None, None, :]
    sine_part = jnp.sin(angles)[:, None, None, :]
    first_half = channels[..., :half_width]
    second_half = channels[..., half_width:]
    return jnp.concatenate([first_half * cosine - second_half * sine_part, second_half * cosine + first_half * sine_part], axis=-1)


def window_mix(queries, key_rows, value_entries, query_pos, key_pos, dilation, reach_rows):
    scores = jnp.einsum('ahc,rhc->har', queries.astype(jnp.float32), key_rows.astype(jnp.float32)) * (queries.shape[-1] ** -0.5)
    distance = query_pos[:, None] - key_pos[None, :]
    allowed = (distance >= 0) & (distance <= reach_rows) & (distance % dilation == 0) & (key_pos[None, :] >= 0)
    scores = jnp.where(allowed[None], scores, -jnp.inf)
    row_max = jnp.max(scores, axis=-1, keepdims=True)
    expo = jnp.where(allowed[None], jnp.exp(scores - row_max), 0.0)
    denominator = jnp.sum(expo, axis=-1)
    rounded = lax.optimization_barrier(expo.astype(jnp.bfloat16)).astype(jnp.float32)
    mixed = jnp.einsum('har,rhc->ahc', rounded, value_entries.astype(jnp.float32))
    mixed = mixed / jnp.transpose(denominator)[:, :, None]
    log_total = jnp.transpose(row_max[..., 0] + jnp.log(denominator))
    return mixed, log_total


def reference(activity, query_weight, key_weight, value_weight, merge_weight):
    tok_total = activity.shape[0]
    local_heads = query_weight.shape[1] // (HEAD_GROUPS * HEAD)
    angle_pos = jnp.arange(tok_total, dtype=jnp.int32).astype(jnp.float32)

    def project(weight):
        return jnp.dot(activity, weight, preferred_element_type=jnp.float32).reshape(tok_total, local_heads, HEAD_GROUPS, HEAD)

    query_all = lax.optimization_barrier(rotate(project(query_weight), angle_pos).astype(jnp.bfloat16))
    key_all = lax.optimization_barrier(rotate(project(key_weight), angle_pos).astype(jnp.bfloat16))
    value_all = lax.optimization_barrier(project(value_weight).astype(jnp.bfloat16))
    group_dilations = (1, DILATION_MIDDLE, DILATION_WIDEST)
    query_groups = []
    padded = []
    for grp_index in range(HEAD_GROUPS):
        reach_rows = SPAN * group_dilations[grp_index]
        query_groups.append(query_all[:, :, grp_index])
        padded.append((jnp.pad(key_all[:, :, grp_index], ((reach_rows, 0), (0, 0), (0, 0))),
                       jnp.pad(value_all[:, :, grp_index], ((reach_rows, 0), (0, 0), (0, 0)))))

    def one_block(block_index):
        start_row = block_index * TOK_DEV
        query_pos = start_row + jnp.arange(TOK_DEV, dtype=jnp.int32)
        mixed_list = []
        total_list = []
        for grp_index in range(HEAD_GROUPS):
            dilation = group_dilations[grp_index]
            reach_rows = SPAN * dilation
            query_blk = lax.dynamic_slice_in_dim(query_groups[grp_index], start_row, TOK_DEV, 0)
            key_blk = lax.dynamic_slice_in_dim(padded[grp_index][0], start_row, reach_rows + TOK_DEV, 0)
            value_blk = lax.dynamic_slice_in_dim(padded[grp_index][1], start_row, reach_rows + TOK_DEV, 0)
            key_pos = start_row - reach_rows + jnp.arange(reach_rows + TOK_DEV, dtype=jnp.int32)
            mixed, log_total = window_mix(query_blk, key_blk, value_blk, query_pos, key_pos, dilation, reach_rows)
            mixed_list.append(mixed)
            total_list.append(log_total)
        total_stack = jnp.stack(total_list)
        peak_total = jnp.max(total_stack, axis=0)
        shifted = jnp.exp(total_stack - peak_total)
        group_weight = shifted / jnp.sum(shifted, axis=0)
        merged = jnp.sum(group_weight[..., None] * jnp.stack(mixed_list), axis=0)
        return merged.astype(jnp.bfloat16).reshape(TOK_DEV, local_heads * HEAD)

    merged_all = lax.map(one_block, jnp.arange(tok_total // TOK_DEV, dtype=jnp.int32))
    merged_all = merged_all.reshape(tok_total, local_heads * HEAD)
    return jnp.dot(merged_all, merge_weight, preferred_element_type=jnp.float32).astype(jnp.bfloat16)
```

```python
import jax
import jax.numpy as jnp
from jax import lax
from jax.experimental import pallas as pl
from jax.experimental.pallas import tpu as pltpu
from jax.sharding import PartitionSpec as P

HEAD = 64
HEAD_GROUPS = 3
SPAN = 128
DILATIONS = (1, 4, 8)
LANES = 128
WIDTH = HEAD_GROUPS * HEAD
PAIR = 2 * WIDTH
ROPE_BASE = 500000.0


VMEM = pltpu.CompilerParams(vmem_limit_bytes=60 * 1024 * 1024)


def whole(shape):
    return pl.BlockSpec(shape, lambda *_: (0,) * len(shape))


HBM = pl.BlockSpec(memory_space=pl.ANY)
SMEM = pl.BlockSpec(memory_space=pltpu.SMEM)


def pack_weights(query_weight, key_weight, value_weight, ring, ids):
    rows, cols = query_weight.shape
    count = max(1, min(4, rows // 32))
    kv_rows, q_rows = rows // count, rows // 2 // count

    def body(ids_ref, q_top, q_low, k_ref, v_ref, *outs):
        home = ids_ref[0]
        for target in range(ring):
            step = lax.rem(target - home + ring, ring)
            cut = slice(target * WIDTH, (target + 1) * WIDTH)
            for d in range(ring):

                @pl.when(step == d)
                def _():
                    outs[d][:, :WIDTH] = k_ref[:, cut]
                    outs[d][:, WIDTH:] = v_ref[:, cut]
                    outs[ring + d][:, :WIDTH] = q_top[:, cut]
                    outs[ring + d][:, WIDTH:] = q_low[:, cut]

    outs = pl.pallas_call(
        body,
        grid=(count,),
        in_specs=[
            SMEM,
            pl.BlockSpec((q_rows, cols), lambda c: (c, 0)),
            pl.BlockSpec((q_rows, cols), lambda c: (c + count, 0)),
            pl.BlockSpec((kv_rows, cols), lambda c: (c, 0)),
            pl.BlockSpec((kv_rows, cols), lambda c: (c, 0)),
        ],
        out_specs=[pl.BlockSpec((kv_rows, PAIR), lambda c: (c, 0))] * ring
        + [pl.BlockSpec((q_rows, PAIR), lambda c: (c, 0))] * ring,
        out_shape=[jax.ShapeDtypeStruct((rows, PAIR), jnp.bfloat16)] * ring
        + [jax.ShapeDtypeStruct((rows // 2, PAIR), jnp.bfloat16)] * ring,
        compiler_params=VMEM,
        name="pack_weights",
    )(ids, query_weight, query_weight, key_weight, value_weight)
    return outs[:ring], outs[ring:]


def turn(x, cosine, sine):
    lane = lax.broadcasted_iota(jnp.int32, x.shape, 1)
    half = HEAD // 2
    swapped = jnp.where(
        lax.rem(lane, HEAD) < half, pltpu.roll(x, LANES - half, 1), pltpu.roll(x, half, 1)
    )
    return x * cosine + swapped * sine


def project(kind, pieces, weights, cosine, sine, ids, ring, others, devices):
    tok, feat = pieces[0][0].shape
    width = feat * len(pieces)
    rows = width // devices
    flat_a = [piece for group in pieces for piece in group]
    flat_w = [piece for group in weights for piece in group]
    count_a, count_w = len(flat_a), len(flat_w)
    out_lanes = PAIR if kind == "kv" else 2 * LANES

    def body(ids_ref, cos_ref, sin_ref, *refs):
        a_refs, refs = refs[:count_a], refs[count_a:]
        w_refs, refs = refs[:count_w], refs[count_w:]
        out_ref, a_buf, w_in, w_buf, a_sem, w_sem = refs
        home, lane_pos, part = ids_ref[0], ids_ref[1], ids_ref[2]
        w_copies, a_copies = [], []
        for d in range(ring):
            for j in range(others):
                block = lax.rem(home - d + ring, ring) * others + lax.rem(lane_pos - j + others, others)
                index = d * others + j
                copy = pltpu.make_async_copy(w_refs[index], w_in.at[block], w_sem.at[index])
                copy.start()
                w_copies.append(copy)
        for k in range(ring):
            for m in range(len(pieces)):
                start = pl.multiple_of((part ^ m) * feat, feat)
                index = m * ring + k
                copy = pltpu.make_async_copy(
                    a_refs[index], a_buf.at[k, :, pl.ds(start, feat)], a_sem.at[index]
                )
                copy.start()
                a_copies.append(copy)
        for copy in w_copies:
            copy.wait()
        if kind == "q":
            w_buf[...] = jnp.zeros_like(w_buf)

            def spread(block, carry):
                top = pl.multiple_of(block * rows, rows)
                low = pl.multiple_of(block * rows + rows // 2, rows // 2)
                w_buf[pl.ds(top, rows // 2), :WIDTH] = w_in[block, :, :WIDTH]
                w_buf[pl.ds(low, rows // 2), :WIDTH] = w_in[block, :, WIDTH:]
                return carry

            lax.fori_loop(0, devices, spread, 0)
        for k in range(ring):
            for copy in a_copies[k * len(pieces) : (k + 1) * len(pieces)]:
                copy.wait()
            block = ids_ref[3 + k]
            weight = w_buf[...] if kind == "q" else w_in[...].reshape(width, PAIR)
            total = jnp.dot(a_buf[k], weight, preferred_element_type=jnp.float32)
            cosine, sine = cos_ref[block], sin_ref[block]
            first = turn(total[:, :LANES], cosine, sine)
            second = turn(total[:, LANES : 2 * LANES], cosine, sine)
            if kind == "q":
                scale = HEAD ** (-0.5)
                out_ref[block, :, :LANES] = (first * scale).astype(jnp.bfloat16)
                out_ref[block, :, LANES:] = (second * scale).astype(jnp.bfloat16)
            else:
                lane = lax.broadcasted_iota(jnp.int32, second.shape, 1)
                second = jnp.where(lane < WIDTH - LANES, second, total[:, LANES : 2 * LANES])
                out_ref[block, :, :LANES] = first.astype(jnp.bfloat16)
                out_ref[block, :, LANES : 2 * LANES] = second.astype(jnp.bfloat16)
                out_ref[block, :, 2 * LANES :] = total[:, 2 * LANES :].astype(jnp.bfloat16)

    w_rows = flat_w[0].shape[0]
    return pl.pallas_call(
        body,
        in_specs=[SMEM, whole(cosine.shape), whole(sine.shape)] + [HBM] * (count_a + count_w),
        out_specs=whole((ring, tok, out_lanes)),
        out_shape=jax.ShapeDtypeStruct((ring, tok, out_lanes), jnp.bfloat16),
        scratch_shapes=[
            pltpu.VMEM((ring, tok, width), jnp.bfloat16),
            pltpu.VMEM((devices, w_rows, PAIR), jnp.bfloat16),
            pltpu.VMEM((width, 2 * LANES) if kind == "q" else (16, LANES), jnp.bfloat16),
            pltpu.SemaphoreType.DMA((count_a,)),
            pltpu.SemaphoreType.DMA((count_w,)),
        ],
        compiler_params=VMEM,
        grid=(1,),
        name="project_" + kind,
    )(ids, cosine, sine, *flat_a, *flat_w)


def attend(queries, kv_own, kv_others, ids, ring, others):
    tok = queries.shape[1]
    back = -(-SPAN * DILATIONS[-1] // tok)
    length = (back + 1) * tok
    widths = [SPAN * dilation + tok for dilation in DILATIONS]
    count = len(kv_others)

    def body(ids_ref, q_ref, own_ref, *refs):
        other_refs, refs = refs[:count], refs[count:]
        out_ref, kv_buf, *bias_refs = refs
        i = pl.program_id(0)
        spot = ids_ref[1]
        position = (i * others + spot) * tok

        @pl.when(i == 0)
        def _():
            for bias_ref, width, dilation in zip(bias_refs, widths, DILATIONS):
                gap = (
                    width
                    - tok
                    + lax.broadcasted_iota(jnp.int32, (tok, width), 0)
                    - lax.broadcasted_iota(jnp.int32, (tok, width), 1)
                )
                allowed = (gap >= 0) & (gap <= SPAN * dilation) & (gap & (dilation - 1) == 0)
                bias_ref[...] = jnp.where(allowed, 0.0, -jnp.inf)

        for j in range(back + 1):
            source = own_ref if j % others == 0 else other_refs[j % others - 1]
            index = i + jnp.floor_divide(spot - j + others * (back + 1), others) - (back + 1)
            rows = slice((back - j) * tok, (back - j + 1) * tok)

            @pl.when(index >= 0)
            def _():
                kv_buf[rows, :] = source[index]

            @pl.when(index < 0)
            def _():
                kv_buf[rows, :] = jnp.zeros((tok, PAIR), jnp.bfloat16)

        lane = lax.broadcasted_iota(jnp.int32, (tok, LANES), 1)
        low = lane < HEAD
        q_first, q_second = q_ref[0, :, :LANES], q_ref[0, :, LANES:]
        zero = jnp.zeros_like(q_first)
        q_groups = (jnp.where(low, q_first, zero), jnp.where(low, zero, q_first), q_second)
        k_lanes = (0, 0, 1)
        v_lanes = (1, 2, 2)
        scores = []
        for group in range(HEAD_GROUPS):
            width = widths[group]
            keys = kv_buf[length - width :, k_lanes[group] * LANES : (k_lanes[group] + 1) * LANES]
            found = lax.dot_general(
                q_groups[group], keys, (((1,), (1,)), ((), ())), preferred_element_type=jnp.float32
            )
            key_pos = position + tok - width + lax.broadcasted_iota(jnp.int32, (1, width), 1)
            found = found + bias_refs[group][...] + jnp.where(key_pos >= 0, 0.0, -jnp.inf)
            scores.append(found)
        peak = jnp.max(scores[0], axis=1, keepdims=True)
        for found in scores[1:]:
            peak = jnp.maximum(peak, jnp.max(found, axis=1, keepdims=True))
        below = jnp.zeros((tok, 1), jnp.float32)
        mixed = []
        for group in range(HEAD_GROUPS):
            width = widths[group]
            expo = jnp.exp(scores[group] - peak)
            below = below + jnp.sum(expo, axis=1, keepdims=True)
            values = kv_buf[length - width :, v_lanes[group] * LANES : (v_lanes[group] + 1) * LANES]
            mixed.append(
                jnp.dot(expo.astype(jnp.bfloat16), values, preferred_element_type=jnp.float32)
            )
        merged = (pltpu.roll(mixed[0] + mixed[2], LANES - HEAD, 1) + mixed[1]) / below
        out_ref[0] = jnp.transpose(merged)[:HEAD].astype(jnp.bfloat16)

    return pl.pallas_call(
        body,
        grid=(ring,),
        in_specs=[
            SMEM,
            pl.BlockSpec((1, tok, 2 * LANES), lambda i: (i, 0, 0)),
            whole(kv_own.shape),
        ]
        + [whole(kv.shape) for kv in kv_others],
        out_specs=pl.BlockSpec((1, HEAD, tok), lambda i: (i, 0, 0)),
        out_shape=jax.ShapeDtypeStruct((ring, HEAD, tok), jnp.bfloat16),
        scratch_shapes=[pltpu.VMEM((length, PAIR), jnp.bfloat16)]
        + [pltpu.VMEM((tok, width), jnp.float32) for width in widths],
        compiler_params=VMEM,
        name="attend",
    )(ids, queries, kv_own, *kv_others)


def merge_heads(heads, weights, ids, ring, others, parts, devices):
    low = max(1, parts // 2)
    tok = heads[0].shape[1]
    share = tok // parts
    flat_w = [piece for group in weights for piece in group]
    rows, cols = flat_w[0].shape[1:]
    count_h, count_w = len(heads), len(flat_w)
    pieces = count_w * ring

    def body(ids_ref, *refs):
        h_refs, refs = refs[:count_h], refs[count_h:]
        w_refs, refs = refs[:count_w], refs[count_w:]
        keep_ref, send_ref, w_buf, side, flat, sems = refs
        home, spot, part = ids_ref[0], ids_ref[1], ids_ref[2]
        copies = []
        for j in range(others):
            for m in range(low):
                for d in range(ring):
                    block = lax.rem(home - d + ring, ring) * others + lax.rem(spot - j + others, others)
                    top = pl.multiple_of(((part ^ m) & (low - 1)) * rows, rows)
                    left = pl.multiple_of(block * cols, cols)
                    index = j * low + m
                    copy = pltpu.make_async_copy(
                        w_refs[index].at[d],
                        w_buf.at[pl.ds(top, rows), pl.ds(left, cols)],
                        sems.at[index * ring + d],
                    )
                    copy.start()
                    copies.append(copy)
        for m in range(low):
            for d in range(ring):
                head = ((part ^ m) & (low - 1)) * ring + lax.rem(home - d + ring, ring)
                top = pl.multiple_of(head * HEAD, HEAD)
                side[pl.ds(top, HEAD), :] = h_refs[m][d * HEAD : (d + 1) * HEAD, :]
        flat[...] = jnp.transpose(side[...].astype(jnp.float32)).astype(jnp.bfloat16)
        mine = flat[pl.ds(pl.multiple_of(part * share, share), share), :]
        theirs = flat[pl.ds(pl.multiple_of((part ^ low) * share, share), share), :]
        both = jnp.concatenate([mine, theirs], axis=0)
        for copy in copies:
            copy.wait()
        total = jnp.dot(both, w_buf[...], preferred_element_type=jnp.float32)
        keep_ref[...] = total[:share]
        send_ref[...] = total[share:].astype(jnp.bfloat16)

    return pl.pallas_call(
        body,
        grid=(1,),
        in_specs=[SMEM] + [whole(head.shape) for head in heads] + [HBM] * count_w,
        out_specs=[whole((share, cols * devices))] * 2,
        out_shape=[
            jax.ShapeDtypeStruct((share, cols * devices), jnp.float32),
            jax.ShapeDtypeStruct((share, cols * devices), jnp.bfloat16),
        ],
        scratch_shapes=[
            pltpu.VMEM((low * rows, cols * devices), jnp.bfloat16),
            pltpu.VMEM((low * ring * HEAD, tok), jnp.bfloat16),
            pltpu.VMEM((tok, low * ring * HEAD), jnp.bfloat16),
            pltpu.SemaphoreType.DMA((pieces,)),
        ],
        compiler_params=VMEM,
        name="merge_heads",
    )(ids, *heads, *flat_w)


def per_device(activity, query_weight, key_weight, value_weight, merge_weight):
    devices, parts = lax.axis_size("sp"), lax.axis_size("tp")
    tok = activity.shape[0]
    ring = query_weight.shape[1] // WIDTH
    others = devices // ring
    place, part = lax.axis_index("sp"), lax.axis_index("tp")
    home, spot = place // others, place % others

    def shift(value, step):
        pairs = [
            (s, (s // others + step) % ring * others + s % others) for s in range(devices)
        ]
        return lax.ppermute(value, "sp", pairs)

    def pass_on(value, step):
        pairs = [
            (s, s + step * others)
            for s in range(devices)
            if 0 <= s // others + step < ring
        ]
        return lax.ppermute(value, "sp", pairs)

    def turn_round(value, step):
        pairs = [(s, s // others * others + (s + step) % others) for s in range(devices)]
        return lax.ppermute(value, "sp", pairs)

    def across(value, bit):
        return lax.ppermute(value, "tp", [(t, t ^ bit) for t in range(parts)])

    table = []
    for at in range(ring):
        order = [("up", 0, at)]
        for d in range(1, ring):
            if at - d >= 0:
                order.append(("up", d, at - d))
            if at + d < ring:
                order.append(("down", d, at + d))
        table.append(order)
    blocks = jnp.array([[entry[2] for entry in order] for order in table], jnp.int32)
    ids = jnp.concatenate(
        [jnp.stack([home, spot, part]).astype(jnp.int32), lax.dynamic_index_in_dim(blocks, home, 0, False)]
    )

    flows = {("up", 0): activity, ("down", 0): activity}
    for d in range(1, ring):
        flows["up", d] = pass_on(flows["up", d - 1], 1)
        flows["down", d] = pass_on(flows["down", d - 1], -1)
    slots = []
    for k in range(ring):
        names = sorted({order[k][:2] for order in table})
        chosen = flows[names[0]]
        for name in names[1:]:
            here = jnp.array([order[k][:2] == name for order in table])
            chosen = jnp.where(here[home], flows[name], chosen)
        slots.append(chosen)
    pieces = {0: slots}
    bit = parts // 2
    while bit:
        for m in list(pieces):
            pieces[m ^ bit] = [across(piece, bit) for piece in pieces[m]]
        bit //= 2
    pieces = [pieces[m] for m in range(parts)]

    packed_kv, packed_q = pack_weights(query_weight, key_weight, value_weight, ring, ids)

    def spread(packed):
        steps = [packed[0]] + [shift(packed[d], d) for d in range(1, ring)]
        return [[piece] + [turn_round(piece, j) for j in range(1, others)] for piece in steps]

    kv_weights, q_weights = spread(packed_kv), spread(packed_q)

    position = (
        (jnp.arange(ring, dtype=jnp.int32) * others + spot)[:, None] * tok
        + jnp.arange(tok, dtype=jnp.int32)[None, :]
    ).astype(jnp.float32)
    half = HEAD // 2
    frequency = ROPE_BASE ** (-jnp.arange(0, half, dtype=jnp.float32) * 2.0 / HEAD)
    angles = position[:, :, None] * frequency[None, None, :]
    cosine, sine = jnp.cos(angles), jnp.sin(angles)
    cosine = jnp.concatenate([cosine] * (LANES // half), axis=-1)
    sine = jnp.concatenate([-sine, sine] * (LANES // HEAD), axis=-1)

    kv_own = project("kv", pieces, kv_weights, cosine, sine, ids, ring, others, devices)
    back = -(-SPAN * DILATIONS[-1] // tok)
    kv_others = [turn_round(kv_own, j) for j in range(1, min(back, others - 1) + 1)]
    queries = project("q", pieces, q_weights, cosine, sine, ids, ring, others, devices)

    merge_steps = jnp.stack([merge_weight] + [shift(merge_weight, d) for d in range(1, ring)])
    merge_pieces = [[merge_steps]] + [[turn_round(merge_steps, j)] for j in range(1, others)]
    bit = 1
    while bit < parts // 2:
        for group in merge_pieces:
            group.extend([across(piece, bit) for piece in group])
        bit *= 2

    merged = attend(queries, kv_own, kv_others, ids, ring, others)
    heads = [lax.dynamic_index_in_dim(merged, home, 0, False)]
    for d in range(1, ring):
        heads.append(shift(lax.dynamic_index_in_dim(merged, (home + d) % ring, 0, False), d))
    heads = [jnp.concatenate(heads, axis=0)]
    bit = 1
    while bit < parts // 2:
        heads.extend([across(piece, bit) for piece in heads])
        bit *= 2
    keep, send = merge_heads(heads, merge_pieces, ids, ring, others, parts, devices)
    return (keep + across(send, parts // 2).astype(jnp.float32)).astype(jnp.bfloat16)


def solution(mesh):
    placed = (P("sp", "tp"), P("sp", "tp"), P("sp", "tp"), P("sp", "tp"), P("tp", "sp"))
    return jax.shard_map(
        per_device, mesh=mesh, in_specs=placed, out_specs=P(("sp", "tp"), None), check_vma=False
    )
```

```python
import functools

import jax
import jax.numpy as jnp
from jax import lax
from jax.experimental import pallas as pl
from jax.experimental.pallas import tpu as pltpu
from jax.sharding import PartitionSpec as P


HEAD = 64
HEAD_GROUPS = 3
SPAN = 128
DILATIONS = (1, 4, 8)
LANES = 128
WIDTH = HEAD_GROUPS * HEAD
PAIR = 2 * WIDTH
ROPE_BASE = 500000.0


VMEM = pltpu.CompilerParams(vmem_limit_bytes=60 * 1024 * 1024)


def whole(shape):
    return pl.BlockSpec(shape, lambda *_: (0,) * len(shape))


HBM = pl.BlockSpec(memory_space=pltpu.HBM)
SMEM = pl.BlockSpec(memory_space=pltpu.SMEM)


def choose(flows, places, ids):
    def body(ids_ref, *refs):
        out_ref, sem = refs[-2:]
        for flow, hosts in zip(refs[:-2], places):
            here = functools.reduce(jnp.logical_or, [ids_ref[0] == at for at in hosts])

            @pl.when(here)
            def _():
                copy = pltpu.make_async_copy(flow, out_ref, sem)
                copy.start()
                copy.wait()

    return pl.pallas_call(
        body,
        in_specs=[SMEM] + [HBM] * len(flows),
        out_specs=HBM,
        out_shape=jax.ShapeDtypeStruct(flows[0].shape, flows[0].dtype),
        scratch_shapes=[pltpu.SemaphoreType.DMA],
        name="choose",
    )(ids, *flows)


def pack_weights(query_weight, key_weight, value_weight, ring, ids):
    rows, cols = query_weight.shape
    count = max(1, min(4, rows // 32))
    kv_rows, q_rows = rows // count, rows // 2 // count

    def body(ids_ref, q_top, q_low, k_ref, v_ref, *outs):
        home = ids_ref[0]
        for target in range(ring):
            step = lax.rem(target - home + ring, ring)
            cut = slice(target * WIDTH, (target + 1) * WIDTH)
            for d in range(ring):

                @pl.when(step == d)
                def _():
                    outs[d][:, :WIDTH] = k_ref[:, cut]
                    outs[d][:, WIDTH:] = v_ref[:, cut]
                    outs[ring + d][:, :WIDTH] = q_top[:, cut]
                    outs[ring + d][:, WIDTH:] = q_low[:, cut]

    outs = pl.pallas_call(
        body,
        grid=(count,),
        in_specs=[
            SMEM,
            pl.BlockSpec((q_rows, cols), lambda c: (c, 0)),
            pl.BlockSpec((q_rows, cols), lambda c: (c + count, 0)),
            pl.BlockSpec((kv_rows, cols), lambda c: (c, 0)),
            pl.BlockSpec((kv_rows, cols), lambda c: (c, 0)),
        ],
        out_specs=[pl.BlockSpec((kv_rows, PAIR), lambda c: (c, 0))] * ring
        + [pl.BlockSpec((q_rows, PAIR), lambda c: (c, 0))] * ring,
        out_shape=[jax.ShapeDtypeStruct((rows, PAIR), jnp.bfloat16)] * ring
        + [jax.ShapeDtypeStruct((rows // 2, PAIR), jnp.bfloat16)] * ring,
        compiler_params=VMEM,
        name="pack_weights",
    )(ids, query_weight, query_weight, key_weight, value_weight)
    return outs[:ring], outs[ring:]


def turn(x, cosine, sine):
    lane = lax.broadcasted_iota(jnp.int32, x.shape, 1)
    half = HEAD // 2
    swapped = jnp.where(
        lax.rem(lane, HEAD) < half, pltpu.roll(x, LANES - half, 1), pltpu.roll(x, half, 1)
    )
    return x * cosine + swapped * sine


def project(kind, pieces, weights, cosine, sine, ids, ring, others, devices):
    tok, feat = pieces[0][0].shape
    parts = len(pieces)
    rows = feat * parts // devices
    share = devices // parts
    flat_a = [piece for group in pieces for piece in group]
    flat_w = [piece for group in weights for piece in group]
    count_a, count_w = len(flat_a), len(flat_w)
    out_lanes = PAIR if kind == "kv" else 2 * LANES

    def body(ids_ref, cos_ref, sin_ref, *refs):
        a_refs, refs = refs[:count_a], refs[count_a:]
        w_refs, refs = refs[:count_w], refs[count_w:]
        out_ref, a_buf, w_in, w_buf, a_sem, w_sem = refs
        home, spot, part = ids_ref[0], ids_ref[1], ids_ref[2]
        w_copies, a_copies = [], []
        for d in range(ring):
            for j in range(others):
                block = lax.rem(home - d + ring, ring) * others + lax.rem(spot - j + others, others)
                index = d * others + j
                copy = pltpu.make_async_copy(w_refs[index], w_in.at[block], w_sem.at[index])
                copy.start()
                w_copies.append(copy)
        for m in range(parts):
            for k in range(ring):
                index = m * ring + k
                copy = pltpu.make_async_copy(
                    a_refs[index], a_buf.at[m, pl.ds(k * tok, tok), :], a_sem.at[index]
                )
                copy.start()
                a_copies.append(copy)
        if kind == "q":
            w_buf[...] = jnp.zeros_like(w_buf)
        for copy in w_copies:
            copy.wait()
        total = None
        for m in range(parts):
            first = (part ^ m) * share
            if kind == "q":

                def spread(n, carry):
                    top = pl.multiple_of(n * rows, rows)
                    low = pl.multiple_of(n * rows + rows // 2, rows // 2)
                    w_buf[pl.ds(top, rows // 2), :WIDTH] = w_in[first + n, :, :WIDTH]
                    w_buf[pl.ds(low, rows // 2), :WIDTH] = w_in[first + n, :, WIDTH:]
                    return carry

                lax.fori_loop(0, share, spread, 0)
                weight = w_buf[...]
            else:
                weight = w_in[pl.ds(first, share)].reshape(feat, PAIR)
            for copy in a_copies[m * ring : (m + 1) * ring]:
                copy.wait()
            found = jnp.dot(a_buf[m], weight, preferred_element_type=jnp.float32)
            total = found if total is None else total + found
        for k in range(ring):
            block = ids_ref[3 + k]
            here = total[k * tok : (k + 1) * tok]
            cosine, sine = cos_ref[block], sin_ref[block]
            first = turn(here[:, :LANES], cosine, sine)
            second = turn(here[:, LANES : 2 * LANES], cosine, sine)
            if kind == "q":
                scale = HEAD ** (-0.5)
                out_ref[block, :, :LANES] = (first * scale).astype(jnp.bfloat16)
                out_ref[block, :, LANES:] = (second * scale).astype(jnp.bfloat16)
            else:
                lane = lax.broadcasted_iota(jnp.int32, second.shape, 1)
                second = jnp.where(lane < WIDTH - LANES, second, here[:, LANES : 2 * LANES])
                out_ref[block, :, :LANES] = first.astype(jnp.bfloat16)
                out_ref[block, :, LANES : 2 * LANES] = second.astype(jnp.bfloat16)
                out_ref[block, :, 2 * LANES :] = here[:, 2 * LANES :].astype(jnp.bfloat16)

    w_rows = flat_w[0].shape[0]
    return pl.pallas_call(
        body,
        in_specs=[SMEM, whole(cosine.shape), whole(sine.shape)] + [HBM] * (count_a + count_w),
        out_specs=whole((ring, tok, out_lanes)),
        out_shape=jax.ShapeDtypeStruct((ring, tok, out_lanes), jnp.bfloat16),
        scratch_shapes=[
            pltpu.VMEM((parts, ring * tok, feat), jnp.bfloat16),
            pltpu.VMEM((devices, w_rows, PAIR), jnp.bfloat16),
            pltpu.VMEM((feat, 2 * LANES) if kind == "q" else (16, LANES), jnp.bfloat16),
            pltpu.SemaphoreType.DMA((count_a,)),
            pltpu.SemaphoreType.DMA((count_w,)),
        ],
        compiler_params=VMEM,
        grid=(1,),
    )(ids, cosine, sine, *flat_a, *flat_w)


def attend(queries, kv_own, kv_others, ids, ring, others):
    tok = queries.shape[1]
    back = -(-SPAN * DILATIONS[-1] // tok)
    length = (back + 1) * tok
    widths = [SPAN * dilation + tok for dilation in DILATIONS]
    count = len(kv_others)

    def body(ids_ref, q_ref, own_ref, *refs):
        other_refs, refs = refs[:count], refs[count:]
        out_ref, kv_buf, *bias_refs = refs
        i = pl.program_id(0)
        spot = ids_ref[1]
        position = (i * others + spot) * tok

        @pl.when(i == 0)
        def _():
            for bias_ref, width, dilation in zip(bias_refs, widths, DILATIONS):
                gap = (
                    width
                    - tok
                    + lax.broadcasted_iota(jnp.int32, (tok, width), 0)
                    - lax.broadcasted_iota(jnp.int32, (tok, width), 1)
                )
                allowed = (gap >= 0) & (gap <= SPAN * dilation) & (gap & (dilation - 1) == 0)
                bias_ref[...] = jnp.where(allowed, 0.0, -jnp.inf)

        for j in range(back + 1):
            source = own_ref if j % others == 0 else other_refs[j % others - 1]
            index = i + jnp.floor_divide(spot - j + others * (back + 1), others) - (back + 1)
            rows = slice((back - j) * tok, (back - j + 1) * tok)

            @pl.when(index >= 0)
            def _():
                kv_buf[rows, :] = source[index]

            @pl.when(index < 0)
            def _():
                kv_buf[rows, :] = jnp.zeros((tok, PAIR), jnp.bfloat16)

        lane = lax.broadcasted_iota(jnp.int32, (tok, LANES), 1)
        low = lane < HEAD
        q_first, q_second = q_ref[0, :, :LANES], q_ref[0, :, LANES:]
        zero = jnp.zeros_like(q_first)
        q_groups = (jnp.where(low, q_first, zero), jnp.where(low, zero, q_first), q_second)
        k_lanes = (0, 0, 1)
        v_lanes = (1, 2, 2)
        scores = []
        for group in range(HEAD_GROUPS):
            width = widths[group]
            keys = kv_buf[length - width :, k_lanes[group] * LANES : (k_lanes[group] + 1) * LANES]
            found = lax.dot_general(
                q_groups[group], keys, (((1,), (1,)), ((), ())), preferred_element_type=jnp.float32
            )
            key_pos = position + tok - width + lax.broadcasted_iota(jnp.int32, (1, width), 1)
            found = found + bias_refs[group][...] + jnp.where(key_pos >= 0, 0.0, -jnp.inf)
            scores.append(found)
        peak = jnp.max(scores[0], axis=1, keepdims=True)
        for found in scores[1:]:
            peak = jnp.maximum(peak, jnp.max(found, axis=1, keepdims=True))
        below = jnp.zeros((tok, 1), jnp.float32)
        mixed = []
        for group in range(HEAD_GROUPS):
            width = widths[group]
            expo = jnp.exp(scores[group] - peak)
            below = below + jnp.sum(expo, axis=1, keepdims=True)
            values = kv_buf[length - width :, v_lanes[group] * LANES : (v_lanes[group] + 1) * LANES]
            mixed.append(
                jnp.dot(expo.astype(jnp.bfloat16), values, preferred_element_type=jnp.float32)
            )
        merged = (pltpu.roll(mixed[0] + mixed[2], LANES - HEAD, 1) + mixed[1]) / below
        out_ref[0] = jnp.transpose(merged)[:HEAD].astype(jnp.bfloat16)

    return pl.pallas_call(
        body,
        grid=(ring,),
        in_specs=[
            SMEM,
            pl.BlockSpec((1, tok, 2 * LANES), lambda i: (i, 0, 0)),
            whole(kv_own.shape),
        ]
        + [whole(kv.shape) for kv in kv_others],
        out_specs=pl.BlockSpec((1, HEAD, tok), lambda i: (i, 0, 0)),
        out_shape=jax.ShapeDtypeStruct((ring, HEAD, tok), jnp.bfloat16),
        scratch_shapes=[pltpu.VMEM((length, PAIR), jnp.bfloat16)]
        + [pltpu.VMEM((tok, width), jnp.float32) for width in widths],
        compiler_params=VMEM,
        name="attend",
    )(ids, queries, kv_own, *kv_others)


def merge_heads(heads, weights, ids, ring, others, parts, devices):
    low = max(1, parts // 2)
    tok = heads[0].shape[1]
    share = tok // parts
    flat_w = [piece for step in weights for group in step for piece in group]
    rows, cols = flat_w[0].shape
    count_h, count_w = len(heads), len(flat_w)

    def body(ids_ref, *refs):
        h_refs, refs = refs[:count_h], refs[count_h:]
        w_refs, refs = refs[:count_w], refs[count_w:]
        keep_ref, send_ref, w_buf, side, flat, sems = refs
        home, spot, part = ids_ref[0], ids_ref[1], ids_ref[2]
        copies = []
        for d in range(ring):
            for j in range(others):
                for m in range(low):
                    block = lax.rem(home - d + ring, ring) * others + lax.rem(spot - j + others, others)
                    top = pl.multiple_of(((part ^ m) & (low - 1)) * rows, rows)
                    left = pl.multiple_of(block * cols, cols)
                    index = (d * others + j) * low + m
                    copy = pltpu.make_async_copy(
                        w_refs[index], w_buf.at[pl.ds(top, rows), pl.ds(left, cols)], sems.at[index]
                    )
                    copy.start()
                    copies.append(copy)
        for m in range(low):
            for d in range(ring):
                head = ((part ^ m) & (low - 1)) * ring + lax.rem(home - d + ring, ring)
                top = pl.multiple_of(head * HEAD, HEAD)
                side[pl.ds(top, HEAD), :] = h_refs[m][d * HEAD : (d + 1) * HEAD, :]
        flat[...] = jnp.transpose(side[...].astype(jnp.float32)).astype(jnp.bfloat16)
        mine = flat[pl.ds(pl.multiple_of(part * share, share), share), :]
        theirs = flat[pl.ds(pl.multiple_of((part ^ low) * share, share), share), :]
        both = jnp.concatenate([mine, theirs], axis=0)
        for copy in copies:
            copy.wait()
        total = jnp.dot(both, w_buf[...], preferred_element_type=jnp.float32)
        keep_ref[...] = total[:share]
        send_ref[...] = total[share:].astype(jnp.bfloat16)

    return pl.pallas_call(
        body,
        grid=(1,),
        in_specs=[SMEM] + [whole(head.shape) for head in heads] + [HBM] * count_w,
        out_specs=[whole((share, cols * devices))] * 2,
        out_shape=[
            jax.ShapeDtypeStruct((share, cols * devices), jnp.float32),
            jax.ShapeDtypeStruct((share, cols * devices), jnp.bfloat16),
        ],
        scratch_shapes=[
            pltpu.VMEM((low * rows, cols * devices), jnp.bfloat16),
            pltpu.VMEM((low * ring * HEAD, tok), jnp.bfloat16),
            pltpu.VMEM((tok, low * ring * HEAD), jnp.bfloat16),
            pltpu.SemaphoreType.DMA((count_w,)),
        ],
        compiler_params=VMEM,
        name="merge_heads",
    )(ids, *heads, *flat_w)


def per_device(activity, query_weight, key_weight, value_weight, merge_weight):
    devices, parts = lax.axis_size("sp"), lax.axis_size("tp")
    tok = activity.shape[0]
    ring = query_weight.shape[1] // WIDTH
    others = devices // ring
    place, part = lax.axis_index("sp"), lax.axis_index("tp")
    home, spot = place // others, place % others

    def shift(value, step):
        pairs = [
            (s, (s // others + step) % ring * others + s % others) for s in range(devices)
        ]
        return lax.ppermute(value, "sp", pairs)

    def pass_on(value, step):
        pairs = [
            (s, s + step * others)
            for s in range(devices)
            if 0 <= s // others + step < ring
        ]
        return lax.ppermute(value, "sp", pairs)

    def turn_round(value, step):
        pairs = [(s, s // others * others + (s + step) % others) for s in range(devices)]
        return lax.ppermute(value, "sp", pairs)

    def across(value, bit):
        return lax.ppermute(value, "tp", [(t, t ^ bit) for t in range(parts)])

    table = []
    for at in range(ring):
        order = [("up", 0, at)]
        for d in range(1, ring):
            if at - d >= 0:
                order.append(("up", d, at - d))
            if at + d < ring:
                order.append(("down", d, at + d))
        table.append(order)
    blocks = jnp.array([[entry[2] for entry in order] for order in table], jnp.int32)
    ids = jnp.concatenate(
        [jnp.stack([home, spot, part]).astype(jnp.int32), lax.dynamic_index_in_dim(blocks, home, 0, False)]
    )

    flows = {("up", 0): activity, ("down", 0): activity}
    for d in range(1, ring):
        flows["up", d] = pass_on(flows["up", d - 1], 1)
        flows["down", d] = pass_on(flows["down", d - 1], -1)
    slots = []
    for k in range(ring):
        names = sorted({order[k][:2] for order in table})
        places = [[at for at in range(ring) if table[at][k][:2] == name] for name in names]
        chosen = activity if k == 0 else choose([flows[name] for name in names], places, ids)
        slots.append(chosen)
    pieces = {0: slots}
    bit = parts // 2
    while bit:
        for m in list(pieces):
            pieces[m ^ bit] = [across(piece, bit) for piece in pieces[m]]
        bit //= 2
    pieces = [pieces[m] for m in range(parts)]

    packed_kv, packed_q = pack_weights(query_weight, key_weight, value_weight, ring, ids)

    def spread(packed):
        steps = [packed[0]] + [shift(packed[d], d) for d in range(1, ring)]
        return [[piece] + [turn_round(piece, j) for j in range(1, others)] for piece in steps]

    kv_weights, q_weights = spread(packed_kv), spread(packed_q)

    position = (
        (jnp.arange(ring, dtype=jnp.int32) * others + spot)[:, None] * tok
        + jnp.arange(tok, dtype=jnp.int32)[None, :]
    ).astype(jnp.float32)
    half = HEAD // 2
    frequency = ROPE_BASE ** (-jnp.arange(0, half, dtype=jnp.float32) * 2.0 / HEAD)
    angles = position[:, :, None] * frequency[None, None, :]
    cosine, sine = jnp.cos(angles), jnp.sin(angles)
    cosine = jnp.concatenate([cosine] * (LANES // half), axis=-1)
    sine = jnp.concatenate([-sine, sine] * (LANES // HEAD), axis=-1)

    kv_own = project("kv", pieces, kv_weights, cosine, sine, ids, ring, others, devices)
    back = -(-SPAN * DILATIONS[-1] // tok)
    kv_others = [turn_round(kv_own, j) for j in range(1, min(back, others - 1) + 1)]
    queries = project("q", pieces, q_weights, cosine, sine, ids, ring, others, devices)

    merge_pieces = []
    for d in range(ring):
        piece = shift(merge_weight, d) if d else merge_weight
        merge_pieces.append([[piece]] + [[turn_round(piece, j)] for j in range(1, others)])
        bit = 1
        while bit < parts // 2:
            for group in merge_pieces[d]:
                group.extend([across(piece, bit) for piece in group])
            bit *= 2

    merged = attend(queries, kv_own, kv_others, ids, ring, others)
    heads = [lax.dynamic_index_in_dim(merged, home, 0, False)]
    for d in range(1, ring):
        heads.append(shift(lax.dynamic_index_in_dim(merged, (home + d) % ring, 0, False), d))
    heads = [jnp.concatenate(heads, axis=0)]
    bit = 1
    while bit < parts // 2:
        heads.extend([across(piece, bit) for piece in heads])
        bit *= 2
    keep, send = merge_heads(heads, merge_pieces, ids, ring, others, parts, devices)
    return (keep + across(send, parts // 2).astype(jnp.float32)).astype(jnp.bfloat16)


def solution(mesh):
    placed = (P("sp", "tp"), P("sp", "tp"), P("sp", "tp"), P("sp", "tp"), P("tp", "sp"))

    return jax.shard_map(per_device, mesh=mesh, in_specs=placed, out_specs=P(("sp", "tp"), None), check_vma=False)
```
